32 devices in a mesh: dp: 4 (over y, x), kv: 4 (over z), tp: 2 (over core).
Axes of the slice: x: 2, y: 2, z: 4, core: 2. Of those that a mesh axis runs over, the one named last changes fastest.
Arguments:
- piece_tokens: bfloat16 [256, 2048], P(('dp', 'kv')), parts along dimension 0, may hold values from -6 to 6
- dec_tokens: bfloat16 [192, 4, 2048], P(('dp', 'kv')), parts along dimension 0, may hold values from -6 to 6
- norm_gain: float32 [2048], replicated, may hold values from 0.1 to 1.9
- query_weight: bfloat16 [2048, 1024], P(None, 'tp'), may hold values from -0.375 to 0.375
- key_weight: bfloat16 [2048, 256], P(None, 'tp'), may hold values from -0.125 to 0.125
- value_weight: bfloat16 [2048, 256], P(None, 'tp'), may hold values from -0.125 to 0.125
- gate_weight: bfloat16 [2048, 8], P(None, 'tp'), may hold values from -0.125 to 0.125
- gate_bias: float32 [8], P('tp'), may hold values from 3.4 to 11
- out_weight: bfloat16 [1024, 2048], P('tp'), may hold values from -0.1875 to 0.1875
- out_gain: float32 [2048], replicated, may hold values from 0.1 to 1.9
- past_keys: bfloat16 [4096, 2, 128], P(('dp', 'kv'), 'tp'), parts along dimension 0, may hold values from -41 to 41
- past_values: bfloat16 [4096, 2, 128], P(('dp', 'kv'), 'tp'), parts along dimension 0, may hold values from -6 to 6
- past_gate: float32 [8, 4096], P('tp', ('dp', 'kv')), parts along dimension 1, may hold values from -1024 to 0
- dec_keys: bfloat16 [192, 512, 2, 128], P(('dp', 'kv'), None, 'tp'), parts along dimension 0, may hold values from -41 to 41
- dec_values: bfloat16 [192, 512, 2, 128], P(('dp', 'kv'), None, 'tp'), parts along dimension 0, may hold values from -6 to 6
- dec_gate: float32 [192, 8, 512], P(('dp', 'kv'), 'tp'), parts along dimension 0, may hold values from -512 to 0
- dec_lengths: int32 [192], P(('dp', 'kv')), parts along dimension 0, may hold values from 1 to 512, as said below
Outputs:
- piece_out: bfloat16 [256, 2048], P(('dp', 'kv')), parts along dimension 0
- dec_out: bfloat16 [192, 4, 2048], P(('dp', 'kv')), parts along dimension 0
The draws below stay inside these ranges and needn't reach their ends.
There are 4 independent parts, one for each index of `dp`. The reference program is written for one: setup_inputs(seed, part) draws one part's arguments, and reference() takes and returns one part's arrays. A program takes and returns all parts, laid end to end along the dimension named above; an argument that names none is the same for every part. Nothing has to cross between parts.
Inputs may be any that keep to these rules, and one draw needn't show every extreme that they name: `dec_lengths`: some decoding sequence has all 512 slots live in every draw.
All inputs are finite; a program needn't handle non-finite values.
Results may differ from the reference program's by a relative error of at most 0.015.
Values may be sent and summed in bfloat16 or wider, within the bound.
A program may use at most 64 MiB of HBM per device.

```python
import math
import jax
import jax.numpy as jnp
from jax import lax

D = 2048
QUERY_HEADS = 8
KV_HEADS = 2
HEAD_DIM = 128
PAST_DEV = 256
DEC_NEW = 4
DEC_PAST = 512
PIECE = 64
PAST = 1024
DEC_SEQS = 48
N_TP = 2


def fast_number():
    return QUERY_HEADS // 2


def head_rank(key):
    return jax.random.permutation(jax.random.fold_in(key, 11), QUERY_HEADS)


def gate_rates(key, leading_shape, length_total, block_len, fast_count):
    complete_shape = leading_shape + (QUERY_HEADS, length_total)
    fast_heads = (head_rank(key) < fast_count)[:, None]
    blocks = length_total // block_len
    factor = jnp.exp(jax.random.uniform(jax.random.fold_in(key, 12), leading_shape + (QUERY_HEADS, blocks), jnp.float32, 0.0, math.log(4.0)))
    factor = jnp.repeat(factor, block_len, axis=-1)
    jitter = jnp.exp(jax.random.uniform(jax.random.fold_in(key, 13), complete_shape, jnp.float32, -0.7, 0.7))
    fast_rate = 1.0 / (30.0 + 70.0 * jax.random.uniform(jax.random.fold_in(key, 14), leading_shape + (QUERY_HEADS, 1), jnp.float32))
    stable_value = jnp.where(fast_heads, fast_rate, 0.35 / length_total) * factor * jitter
    outlier_place = jax.random.randint(jax.random.fold_in(key, 15), leading_shape + (QUERY_HEADS, 3), 0, length_total)
    outlier_hit = jnp.any(jnp.arange(length_total) == outlier_place[..., None], axis=-2)
    outlier_size = jnp.where(outlier_hit, jax.random.uniform(jax.random.fold_in(key, 16), complete_shape, jnp.float32, 0.22, 0.45), 0.0)
    return -(stable_value + outlier_size)


def live_lengths(key):
    base_key = jax.random.fold_in(key, 41)
    first_draw = jax.random.randint(jax.random.fold_in(base_key, 1), (DEC_SEQS,), 1, DEC_PAST + 1)
    second_draw = jax.random.randint(jax.random.fold_in(base_key, 2), (DEC_SEQS,), 1, DEC_PAST + 1)
    product = jnp.maximum(first_draw * second_draw // DEC_PAST, 1)
    chosen = jax.random.randint(jax.random.fold_in(base_key, 3), (), 0, DEC_SEQS)
    return jnp.where(jnp.arange(DEC_SEQS) == chosen, DEC_PAST, product).astype(jnp.int32)


def draw_gate_bias(key, part):
    fast_heads = head_rank(key) < fast_number()
    spread = jax.random.uniform(jax.random.fold_in(key, 12), (QUERY_HEADS,), jnp.float32)
    return jnp.where(fast_heads, 3.4 + 1.2 * spread, 9.5 + 1.5 * spread)


def draw_past_keys(key, part):
    noise_rows = jnp.clip(jax.random.normal(jax.random.fold_in(key, 31), (PAST, KV_HEADS, HEAD_DIM), jnp.float32), -6.0, 6.0)
    return noise_rows.astype(jnp.bfloat16)


def draw_past_values(key, part):
    noise_rows = jax.random.normal(jax.random.fold_in(key, 37), (PAST, KV_HEADS, HEAD_DIM), jnp.float32)
    return jnp.clip(noise_rows, -6.0, 6.0).astype(jnp.bfloat16)


def draw_past_gate(key, part):
    gate_step = gate_rates(key, (), PAST, PAST_DEV, fast_number())
    return jnp.flip(jnp.cumsum(jnp.flip(gate_step, -1), -1), -1) - gate_step


def draw_dec_keys(key, part):
    noise_rows = jnp.clip(jax.random.normal(jax.random.fold_in(key, 34), (DEC_SEQS, DEC_PAST, KV_HEADS, HEAD_DIM), jnp.float32), -6.0, 6.0)
    return noise_rows.astype(jnp.bfloat16)


def draw_dec_gate(key, part):
    return jnp.cumsum(gate_rates(key, (DEC_SEQS,), DEC_PAST, DEC_PAST // 4, fast_number()), -1)


def draw_dec_lengths(key, part):
    return live_lengths(key)


def shard_levels(rng, shape, split, least, largest):
    loudness = 1.0
    for axis_at, parts in split:
        steps = jax.random.uniform(jax.random.fold_in(jax.random.fold_in(rng, 6), axis_at), (parts,), jnp.float32, least / len(split), largest / len(split))
        loudness = loudness * jnp.repeat(jnp.exp(steps), shape[axis_at] // parts).reshape((-1,) + (1,) * (len(shape) - 1 - axis_at))
    return loudness


def noise(stream_key, shape, scale, limit, cuts=(), kind=jnp.bfloat16):
    factor_of = shard_levels(stream_key, shape, cuts, -0.22, 0.18) if cuts else 1.0
    drawn = jax.random.normal(stream_key, shape, jnp.float32) * scale * factor_of
    return jnp.minimum(jnp.maximum(drawn, -limit), limit).astype(kind)


def setup_inputs(seed: int = 0, part: int = 0) -> dict:
    key_list = jax.random.split(jax.random.key(seed), 18)
    part_splits = jax.random.split(jax.random.fold_in(key_list[17], part), 18)
    piece_tokens = noise(part_splits[0], (PIECE, D), 1.0, 6.0, ((0, 4),))
    dec_tokens = noise(part_splits[1], (DEC_SEQS, DEC_NEW, D), 1.0, 6.0, ((0, 4),))
    norm_gain = jnp.clip(1.0 + 0.18 * jax.random.normal(key_list[2], (D,), jnp.float32), 0.1, 1.9)
    query_weight = noise(key_list[3], (D, QUERY_HEADS * HEAD_DIM), (D // 9) ** -0.5, 0.375, ((1, 2),))
    key_weight = noise(key_list[4], (D, KV_HEADS * HEAD_DIM), D ** -0.5, 0.125, ((1, 2),))
    value_weight = noise(key_list[5], (D, KV_HEADS * HEAD_DIM), D ** -0.5, 0.125, ((1, 2),))
    gate_weight = noise(key_list[6], (D, QUERY_HEADS), D ** -0.5, 0.125, ((1, 2),))
    gate_bias = draw_gate_bias(jax.random.fold_in(key_list[17], 71), part)
    out_weight = noise(key_list[8], (QUERY_HEADS * HEAD_DIM, D), (QUERY_HEADS * HEAD_DIM) ** -0.5, 0.1875, ((0, 2),))
    out_gain = jnp.clip(1.0 + 0.18 * jax.random.normal(key_list[9], (D,), jnp.float32), 0.1, 1.9)
    past_keys = draw_past_keys(jax.random.fold_in(jax.random.fold_in(key_list[17], part), 71), part)
    past_values = draw_past_values(jax.random.fold_in(jax.random.fold_in(key_list[17], part), 71), part)
    past_gate = draw_past_gate(jax.random.fold_in(jax.random.fold_in(key_list[17], part), 71), part)
    dec_keys = draw_dec_keys(jax.random.fold_in(jax.random.fold_in(key_list[17], part), 71), part)
    dec_values = noise(part_splits[14], (DEC_SEQS, DEC_PAST, KV_HEADS, HEAD_DIM), 1.0, 6.0, ((0, 4), (2, 2)))
    dec_gate = draw_dec_gate(jax.random.fold_in(jax.random.fold_in(key_list[17], part), 71), part)
    dec_lengths = draw_dec_lengths(jax.random.fold_in(jax.random.fold_in(key_list[17], part), 71), part)
    return dict(piece_tokens=piece_tokens, dec_tokens=dec_tokens, norm_gain=norm_gain, query_weight=query_weight, key_weight=key_weight, value_weight=value_weight, gate_weight=gate_weight, gate_bias=gate_bias, out_weight=out_weight, out_gain=out_gain, past_keys=past_keys, past_values=past_values, past_gate=past_gate, dec_keys=dec_keys, dec_values=dec_values, dec_gate=dec_gate, dec_lengths=dec_lengths)


EPS = 1e-06

def rms_scale(source, scale_gain):
    widened = source.astype(jnp.float32)
    return widened * lax.rsqrt(lax.optimization_barrier(jnp.mean(widened * widened, axis=-1, keepdims=True)) + EPS) * scale_gain

def attend(scores, value_block):
    row_top = lax.optimization_barrier(jnp.max(scores, axis=-1, keepdims=True))
    exponent = jnp.exp(scores - row_top)
    weights = exponent.astype(jnp.bfloat16)
    summed = jnp.einsum('gqk,kd->gqd', weights.astype(jnp.float32), value_block.astype(jnp.float32))
    return summed / lax.optimization_barrier(jnp.sum(exponent, axis=-1, keepdims=True))

def reference(piece_tokens, dec_tokens, norm_gain, query_weight, key_weight, value_weight, gate_weight, gate_bias, out_weight, out_gain, past_keys, past_values, past_gate, dec_keys, dec_values, dec_gate, dec_lengths):
    group_size = QUERY_HEADS // KV_HEADS
    score_scale = HEAD_DIM ** (-0.5)
    all_rows = jnp.concatenate([piece_tokens, dec_tokens.reshape(DEC_SEQS * DEC_NEW, D)], axis=0)
    normed = rms_scale(all_rows, norm_gain).astype(jnp.bfloat16)
    queries = jnp.dot(normed, query_weight, preferred_element_type=jnp.float32).astype(jnp.bfloat16)
    key_rows = jnp.dot(normed, key_weight, preferred_element_type=jnp.float32).astype(jnp.bfloat16)
    value_rows = jnp.dot(normed, value_weight, preferred_element_type=jnp.float32).astype(jnp.bfloat16)
    log_gates = jax.nn.log_sigmoid(jnp.dot(normed, gate_weight, preferred_element_type=jnp.float32) + gate_bias)
    piece_queries = queries[:PIECE].reshape(PIECE, KV_HEADS, group_size, HEAD_DIM)
    piece_run = jnp.cumsum(log_gates[:PIECE], axis=0)
    joined_keys = jnp.concatenate([past_keys, key_rows[:PIECE].reshape(PIECE, KV_HEADS, HEAD_DIM)], axis=0).astype(jnp.float32)
    joined_values = jnp.concatenate([past_values, value_rows[:PIECE].reshape(PIECE, KV_HEADS, HEAD_DIM)], axis=0)
    key_bias = jnp.concatenate([past_gate, -piece_run.T], axis=1).reshape(KV_HEADS, group_size, PAST + PIECE)
    block_rows = math.gcd(PIECE, 64)
    key_index = jnp.arange(PAST + PIECE)

    def piece_block(block_start):
        block_queries = lax.dynamic_slice_in_dim(piece_queries, block_start, block_rows, 0).astype(jnp.float32)
        block_run = lax.dynamic_slice_in_dim(piece_run, block_start, block_rows, 0).reshape(block_rows, KV_HEADS, group_size)
        row_place = block_start + jnp.arange(block_rows)
        visible = key_index[None, :] <= PAST + row_place[:, None]
        results = []
        for kv_head in range(KV_HEADS):
            scores = jnp.einsum('bgd,kd->gbk', block_queries[:, kv_head], joined_keys[:, kv_head]) * score_scale
            scores = scores + key_bias[kv_head][:, None, :] + block_run[:, kv_head].T[:, :, None]
            scores = jnp.where(visible[None], scores, -jnp.inf)
            results.append(attend(scores, joined_values[:, kv_head]))
        return jnp.stack(results, axis=0)
    starts = (jnp.arange(PIECE // block_rows) * block_rows).astype(jnp.int32)
    piece_blocks = lax.map(piece_block, starts)
    piece_attention = jnp.transpose(piece_blocks, (0, 3, 1, 2, 4)).reshape(PIECE, QUERY_HEADS * HEAD_DIM).astype(jnp.bfloat16)
    dec_queries = queries[PIECE:].reshape(DEC_SEQS, DEC_NEW, KV_HEADS, group_size, HEAD_DIM)
    dec_new_keys = key_rows[PIECE:].reshape(DEC_SEQS, DEC_NEW, KV_HEADS, HEAD_DIM)
    dec_new_values = value_rows[PIECE:].reshape(DEC_SEQS, DEC_NEW, KV_HEADS, HEAD_DIM)
    dec_run = jnp.cumsum(log_gates[PIECE:].reshape(DEC_SEQS, DEC_NEW, QUERY_HEADS), axis=1)
    slot_index = jnp.arange(DEC_PAST + DEC_NEW)
    new_index = jnp.arange(DEC_NEW)

    def dec_sequence(inputs):
        seq_queries, new_keys, new_values, seq_run, old_keys, old_values, old_gate, length_total = inputs
        last_gate = lax.dynamic_slice_in_dim(old_gate, (length_total - 1).astype(jnp.int32), 1, 1)[:, 0]
        joined = jnp.concatenate([old_keys, new_keys], axis=0).astype(jnp.float32)
        joined_rows = jnp.concatenate([old_values, new_values], axis=0)
        seq_bias = jnp.concatenate([last_gate[:, None] - old_gate, -seq_run.T], axis=1)
        seq_bias = seq_bias.reshape(KV_HEADS, group_size, DEC_PAST + DEC_NEW)
        visible = jnp.where(slot_index[None, :] < DEC_PAST, slot_index[None, :] < length_total, slot_index[None, :] - DEC_PAST <= new_index[:, None])
        row_bias = seq_run.reshape(DEC_NEW, KV_HEADS, group_size)
        results = []
        for kv_head in range(KV_HEADS):
            scores = jnp.einsum('tgd,kd->gtk', seq_queries[:, kv_head].astype(jnp.float32), joined[:, kv_head]) * score_scale
            scores = scores + seq_bias[kv_head][:, None, :] + row_bias[:, kv_head].T[:, :, None]
            scores = jnp.where(visible[None], scores, -jnp.inf)
            results.append(attend(scores, joined_rows[:, kv_head]))
        return jnp.stack(results, axis=0)
    dec_blocks = lax.map(dec_sequence, (dec_queries, dec_new_keys, dec_new_values, dec_run, dec_keys, dec_values, dec_gate, dec_lengths))
    dec_attention = jnp.transpose(dec_blocks, (0, 3, 1, 2, 4)).reshape(DEC_SEQS * DEC_NEW, QUERY_HEADS * HEAD_DIM).astype(jnp.bfloat16)
    attention = jnp.concatenate([piece_attention, dec_attention], axis=0)
    group_width = QUERY_HEADS * HEAD_DIM // N_TP
    mixed = jnp.zeros((attention.shape[0], D), jnp.float32)
    for tp_group in range(N_TP):
        head_partial = jnp.dot(attention[:, tp_group * group_width:(tp_group + 1) * group_width], out_weight[tp_group * group_width:(tp_group + 1) * group_width], preferred_element_type=jnp.float32).astype(jnp.bfloat16)
        mixed = mixed + lax.optimization_barrier(head_partial).astype(jnp.float32)
    final_rows = rms_scale(mixed, out_gain).astype(jnp.bfloat16)
    return (final_rows[:PIECE], final_rows[PIECE:].reshape(DEC_SEQS, DEC_NEW, D))
```

```python
import functools
import math

import jax
import jax.numpy as jnp
from jax import lax
from jax.experimental import pallas as pl
from jax.experimental.pallas import tpu as pltpu
from jax.sharding import PartitionSpec as P

EPS = 1e-06
MESH = pl.DeviceIdType.MESH
F32 = jnp.float32
BF16 = jnp.bfloat16


def dot(a, b):
    return lax.dot_general(a, b, (((1,), (0,)), ((), ())), preferred_element_type=F32)


def dot_t(a, b):
    return lax.dot_general(a, b, (((1,), (1,)), ((), ())), preferred_element_type=F32)


def rms_scale(source, gain):
    return source * lax.rsqrt(jnp.mean(source * source, axis=-1, keepdims=True) + EPS) * gain


def running_sum(rows, period):
    count, lanes = rows.shape
    place = lax.broadcasted_iota(jnp.int32, (count, lanes), 0)
    place = place & (period - 1) if period & (period - 1) == 0 else lax.rem(place, period)
    step = 1
    while step < period:
        shifted = jnp.concatenate([jnp.zeros((step, lanes), F32), rows[: count - step]], axis=0)
        rows = rows + jnp.where(place >= step, shifted, 0.0)
        step *= 2
    return rows


def kernel(
    kv_count,
    tp_count,
    piece_tokens,
    dec_tokens,
    norm_gain,
    query_weight,
    key_weight,
    value_weight,
    gate_weight,
    gate_bias,
    out_weight,
    out_gain,
    past_keys,
    past_values,
    past_gate,
    dec_keys,
    dec_values,
    dec_gate,
    dec_lengths,
    piece_out,
    dec_out,
    v_piece,
    v_dec,
    v_gain,
    v_wq,
    v_wk,
    v_wv,
    v_wg,
    v_bias,
    v_wo,
    v_ogain,
    v_pk,
    v_pv,
    v_pgate,
    v_dk,
    v_dv,
    v_dgate,
    v_len,
    rows_x,
    q_split,
    run_split,
    att_split,
    q_send,
    q_all,
    run_send,
    run_all,
    part_send,
    part_all,
    stat_send,
    stat_all,
    dec_part,
    dec_parts,
    piece_part,
    piece_parts,
    in_sem,
    dk_sem,
    dv_sem,
    q_ssem,
    q_rsem,
    run_ssem,
    run_rsem,
    part_ssem,
    part_rsem,
    stat_ssem,
    stat_rsem,
    tpd_ssem,
    tpd_rsem,
    tpp_ssem,
    tpp_rsem,
):
    R = v_piece.shape[0]
    S, T, D = v_dec.shape
    H = v_bias.shape[1]
    HD = v_pk.shape[1]
    PL = v_pk.shape[0]
    DP = v_dk.shape[1]
    N = S * T
    groups = dk_sem.shape[0]
    G = S // groups
    scale = HD ** (-0.5)
    me = lax.axis_index("kv")
    core = lax.axis_index("tp")

    loads = {}
    pairs = [
        (piece_tokens, v_piece),
        (dec_tokens, v_dec),
        (norm_gain, v_gain),
        (gate_weight, v_wg),
        (gate_bias, v_bias),
        (query_weight, v_wq),
        (key_weight, v_wk),
        (value_weight, v_wv),
        (dec_gate, v_dgate),
        (dec_lengths, v_len),
        (past_gate, v_pgate),
        (past_keys, v_pk),
        (past_values, v_pv),
    ]
    late = [(out_weight, v_wo), (out_gain, v_ogain)]
    count = 0

    def start_load(src, dst):
        nonlocal count
        loads[id(dst)] = pltpu.make_async_copy(src, dst, in_sem.at[count])
        loads[id(dst)].start()
        count += 1

    for src, dst in pairs:
        start_load(src, dst)
    dec_loads = []
    for g in range(groups):
        part = pl.ds(g * G, G)
        ck = pltpu.make_async_copy(dec_keys.at[part], v_dk.at[part], dk_sem.at[g])
        cv = pltpu.make_async_copy(dec_values.at[part], v_dv.at[part], dv_sem.at[g])
        ck.start()
        cv.start()
        dec_loads.append((ck, cv))
    for src, dst in late:
        start_load(src, dst)

    def ready(*refs):
        for ref in refs:
            loads[id(ref)].wait()

    barrier = pltpu.get_barrier_semaphore()
    for i in range(1, kv_count):
        pl.semaphore_signal(
            barrier, inc=1, device_id={"kv": lax.rem(me + i, kv_count)}, device_id_type=MESH
        )
    for i in range(1, tp_count):
        pl.semaphore_signal(
            barrier, inc=1, device_id={"tp": lax.rem(core + i, tp_count)}, device_id_type=MESH
        )

    ready(v_piece, v_dec, v_gain)
    rows_x[:R, :] = v_piece[...].astype(F32)
    for s in range(S):
        rows_x[R + s * T : R + (s + 1) * T, :] = v_dec[s].astype(F32)
    normed = rms_scale(rows_x[...], v_gain[...]).astype(BF16)
    ready(v_wg, v_bias)
    logits = dot_t(normed, v_wg[...]) + v_bias[...]
    log_gates = jnp.minimum(logits, 0.0) - jnp.log1p(jnp.exp(-jnp.abs(logits)))
    log_gates = jnp.concatenate([log_gates, jnp.zeros((R + N, HD - H), F32)], axis=1)
    local_run = running_sum(log_gates[:R], R)
    dec_run = running_sum(log_gates[R:], T)
    run_send[...] = local_run
    ready(v_wq)
    queries = dot(normed, v_wq[...])
    q_send[...] = queries[:R].astype(BF16)
    pl.semaphore_wait(barrier, kv_count - 1 + tp_count - 1)

    def exchange(src_of, dst, ssem, rsem):
        copies = []
        for i in range(1, kv_count):
            peer = lax.rem(me + i, kv_count)
            copy = pltpu.make_async_remote_copy(
                src_ref=src_of(peer),
                dst_ref=dst.at[me],
                send_sem=ssem.at[i - 1],
                recv_sem=rsem.at[i - 1],
                device_id={"kv": peer},
                device_id_type=MESH,
            )
            copy.start()
            copies.append(copy)
        return copies

    q_copies = exchange(lambda peer: q_send, q_all, q_ssem, q_rsem)
    run_copies = exchange(lambda peer: run_send, run_all, run_ssem, run_rsem)
    q_all[me] = queries[:R].astype(BF16)
    run_all[me] = local_run

    for h in range(H):
        q_split[pl.ds(h, N, stride=H), :] = queries[R:, h * HD : (h + 1) * HD]
        run_split[pl.ds(h, N, stride=H), :] = jnp.broadcast_to(dec_run[:, h : h + 1], (N, HD))
    ready(v_wk, v_wv)
    key_rows = dot(normed, v_wk[...]).astype(BF16)
    value_rows = dot(normed, v_wv[...]).astype(BF16)
    pad = -(R + N) % 128
    runs_t = jnp.transpose(
        jnp.concatenate([local_run, dec_run, jnp.zeros((pad, HD), F32)], axis=0)
    )
    local_t = runs_t[:H, :R]
    dec_t = runs_t[:H, R : R + N]

    qd = q_split[...].astype(BF16)
    new_bias = jnp.concatenate([dec_t] * N, axis=0)
    new_scores = dot_t(qd, key_rows[R:]) * scale + run_split[:, :1] - new_bias
    row_at = lax.broadcasted_iota(jnp.int32, (N * H, N), 0)
    col_at = lax.broadcasted_iota(jnp.int32, (N * H, N), 1)
    col_in = col_at & (T - 1) if T & (T - 1) == 0 else lax.rem(col_at, T)
    keep = (row_at >= H * col_at) & (row_at < H * (col_at - col_in + T))
    new_scores = jnp.where(keep, new_scores, -jnp.inf)

    ready(v_dgate, v_len)
    slot = lax.broadcasted_iota(jnp.int32, (H, DP), 1)

    def decode_group(g):
        ck, cv = dec_loads[g]
        lo, hi = g * G * T * H, (g + 1) * G * T * H
        ck.wait()
        biases, scores = [], []
        for s in range(g * G, (g + 1) * G):
            length = v_len[:, s : s + 1]
            gate = v_dgate[s]
            last = jnp.sum(jnp.where(slot == length - 1, gate, 0.0), axis=1, keepdims=True)
            bias = jnp.where(slot < length, last - gate, -jnp.inf)
            biases.append(jnp.concatenate([bias] * T, axis=0))
            scores.append(dot_t(qd[s * T * H : (s + 1) * T * H], v_dk[s]))
        old = jnp.concatenate(scores, axis=0) * scale + run_split[lo:hi, :1]
        old = old + jnp.concatenate(biases, axis=0)
        new = new_scores[lo:hi]
        top = jnp.maximum(
            jnp.max(old, axis=1, keepdims=True), jnp.max(new, axis=1, keepdims=True)
        )
        old = jnp.exp(old - top)
        new = jnp.exp(new - top)
        total = jnp.sum(old, axis=1, keepdims=True) + jnp.sum(new, axis=1, keepdims=True)
        old = old.astype(BF16)
        cv.wait()
        summed = jnp.concatenate(
            [
                dot(old[i * T * H : (i + 1) * T * H], v_dv[g * G + i])
                for i in range(G)
            ],
            axis=0,
        )
        summed = summed + dot(new.astype(BF16), value_rows[R:])
        att_split[lo:hi, :] = summed / total

    early = max(groups - 1, 1)
    for g in range(early):
        decode_group(g)

    ready(v_pgate, v_pk, v_pv)
    for copy in run_copies:
        copy.wait_recv()
    before = jnp.zeros((1, HD), F32)
    own_before = jnp.zeros((1, HD), F32)
    run_rows = []
    for d in range(kv_count):
        shard = run_all[d]
        own_before = jnp.where(me == d, before, own_before)
        run_rows.append(shard + before)
        before = before + shard[R - 1 : R]
    rows_run = jnp.concatenate(run_rows, axis=0)
    M = kv_count * R
    for copy in q_copies:
        copy.wait_recv()
    qp = jnp.concatenate(
        [q_all[:, :, h * HD : (h + 1) * HD].reshape(M, HD) for h in range(H)], axis=0
    )
    row_bias = jnp.concatenate([rows_run[:, h : h + 1] for h in range(H)], axis=0)
    past_bias = jnp.concatenate(
        [jnp.broadcast_to(v_pgate[h : h + 1, :], (M, PL)) for h in range(H)], axis=0
    )
    own_bias = jnp.concatenate(
        [
            jnp.broadcast_to(local_t[h : h + 1, :] + own_before[:, h : h + 1], (M, R))
            for h in range(H)
        ],
        axis=0,
    )
    old = dot_t(qp, v_pk[...]) * scale + past_bias + row_bias
    new = dot_t(qp, key_rows[:R]) * scale + row_bias - own_bias
    causal = me * R + lax.broadcasted_iota(jnp.int32, (M, R), 1) <= lax.broadcasted_iota(
        jnp.int32, (M, R), 0
    )
    causal = jnp.where(causal, 0.0, -jnp.inf)
    new = new + jnp.concatenate([causal] * H, axis=0)
    top = jnp.maximum(jnp.max(old, axis=1, keepdims=True), jnp.max(new, axis=1, keepdims=True))
    old = jnp.exp(old - top)
    new = jnp.exp(new - top)
    total = jnp.sum(old, axis=1, keepdims=True) + jnp.sum(new, axis=1, keepdims=True)
    summed = dot(old.astype(BF16), v_pv[...]) + dot(new.astype(BF16), value_rows[:R])
    lane = lax.broadcasted_iota(jnp.int32, (M, HD), 1)
    stats = jnp.zeros((M, HD), F32)
    for h in range(H):
        part = slice(h * M, (h + 1) * M)
        part_send[:, :, h * HD : (h + 1) * HD] = summed[part].astype(BF16).reshape(kv_count, R, HD)
        stats = jnp.where(lane == h, top[part], stats)
        stats = jnp.where(lane == H + h, total[part], stats)
    stat_send[...] = stats.reshape(kv_count, R, HD)
    part_copies = exchange(lambda peer: part_send.at[peer], part_all, part_ssem, part_rsem)
    stat_copies = exchange(lambda peer: stat_send.at[peer], stat_all, stat_ssem, stat_rsem)
    part_all[me] = part_send[me]
    stat_all[me] = stat_send[me]

    for g in range(early, groups):
        decode_group(g)

    def to_cores(src, dst, ssem, rsem):
        copies = []
        for i in range(1, tp_count):
            copy = pltpu.make_async_remote_copy(
                src_ref=src,
                dst_ref=dst.at[i - 1],
                send_sem=ssem.at[i - 1],
                recv_sem=rsem.at[i - 1],
                device_id={"tp": lax.rem(core + i, tp_count)},
                device_id_type=MESH,
            )
            copy.start()
            copies.append(copy)
        return copies

    ready(v_wo, v_ogain)
    dec_att = jnp.concatenate(
        [att_split[pl.ds(h, N, stride=H), :].astype(BF16) for h in range(H)], axis=1
    )
    dec_part[...] = dot(dec_att, v_wo[...]).astype(BF16)
    tpd_copies = to_cores(dec_part, dec_parts, tpd_ssem, tpd_rsem)

    for copy in stat_copies + part_copies:
        copy.wait_recv()
    stat = [stat_all[d] for d in range(kv_count)]
    best = functools.reduce(jnp.maximum, stat)
    pieces = []
    weights = [jnp.exp(x[:, :H] - best[:, :H]) for x in stat]
    whole = functools.reduce(jnp.add, [x[:, H : 2 * H] * w for x, w in zip(stat, weights)])
    for h in range(H):
        mixed = functools.reduce(
            jnp.add,
            [
                part_all[d, :, h * HD : (h + 1) * HD].astype(F32) * weights[d][:, h : h + 1]
                for d in range(kv_count)
            ],
        )
        pieces.append((mixed / whole[:, h : h + 1]).astype(BF16))
    piece_att = jnp.concatenate(pieces, axis=1)
    piece_part[...] = dot(piece_att, v_wo[...]).astype(BF16)
    tpp_copies = to_cores(piece_part, piece_parts, tpp_ssem, tpp_rsem)

    def finish(part, parts, copies):
        mixed = part[...].astype(F32)
        for i in range(tp_count - 1):
            copies[i].wait_recv()
            mixed = mixed + parts[i].astype(F32)
        return rms_scale(mixed, v_ogain[...])

    final = finish(dec_part, dec_parts, tpd_copies)
    for s in range(S):
        dec_out[s] = final[s * T : (s + 1) * T].astype(BF16)
    piece_out[...] = finish(piece_part, piece_parts, tpp_copies).astype(BF16)
    for copy in q_copies + run_copies + part_copies + stat_copies + tpd_copies + tpp_copies:
        copy.wait_send()


def body(kv_count, tp_count, *args):
    (
        piece_tokens,
        dec_tokens,
        norm_gain,
        query_weight,
        key_weight,
        value_weight,
        gate_weight,
        gate_bias,
        out_weight,
        out_gain,
        past_keys,
        past_values,
        past_gate,
        dec_keys,
        dec_values,
        dec_gate,
        dec_lengths,
    ) = args
    R, D = piece_tokens.shape
    S, T, _ = dec_tokens.shape
    PL, kv_local, HD = past_keys.shape
    DP = dec_keys.shape[1]
    H = gate_bias.shape[0]
    assert kv_local == 1
    N = S * T
    operands = (
        piece_tokens,
        dec_tokens,
        norm_gain.reshape(1, D),
        query_weight,
        key_weight,
        value_weight,
        gate_weight.T,
        gate_bias.reshape(1, H),
        out_weight,
        out_gain.reshape(1, D),
        past_keys.reshape(PL, HD),
        past_values.reshape(PL, HD),
        past_gate,
        dec_keys.reshape(S, DP, HD),
        dec_values.reshape(S, DP, HD),
        dec_gate,
        dec_lengths.reshape(1, S),
    )
    groups = math.gcd(S, 3)
    kv_peers = max(kv_count - 1, 1)
    tp_peers = max(tp_count - 1, 1)
    vmem = pltpu.VMEM
    dma = pltpu.SemaphoreType.DMA
    scratch = [vmem(x.shape, x.dtype) for x in operands] + [
        vmem((R + N, D), F32),
        vmem((N * H, HD), F32),
        vmem((N * H, HD), F32),
        vmem((N * H, HD), F32),
        vmem((R, H * HD), BF16),
        vmem((kv_count, R, H * HD), BF16),
        vmem((R, HD), F32),
        vmem((kv_count, R, HD), F32),
        vmem((kv_count, R, H * HD), BF16),
        vmem((kv_count, R, H * HD), BF16),
        vmem((kv_count, R, HD), F32),
        vmem((kv_count, R, HD), F32),
        vmem((N, D), BF16),
        vmem((tp_peers, N, D), BF16),
        vmem((R, D), BF16),
        vmem((tp_peers, R, D), BF16),
        dma((len(operands),)),
        dma((groups,)),
        dma((groups,)),
    ]
    scratch += [dma((kv_peers,))] * 8 + [dma((tp_peers,))] * 4
    return pl.pallas_call(
        functools.partial(kernel, kv_count, tp_count),
        out_shape=(
            jax.ShapeDtypeStruct((R, D), BF16),
            jax.ShapeDtypeStruct((S, T, D), BF16),
        ),
        in_specs=[pl.BlockSpec(memory_space=pl.ANY)] * len(operands),
        out_specs=(pl.BlockSpec(memory_space=pltpu.VMEM),) * 2,
        scratch_shapes=scratch,
        compiler_params=pltpu.CompilerParams(collective_id=0, has_side_effects=True),
        name="layer",
    )(*operands)


def solution(mesh):
    return jax.shard_map(
        functools.partial(body, mesh.shape["kv"], mesh.shape["tp"]),
        mesh=mesh,
        in_specs=(
            P(("dp", "kv"), None),
            P(("dp", "kv"), None, None),
            P(),
            P(None, "tp"),
            P(None, "tp"),
            P(None, "tp"),
            P(None, "tp"),
            P("tp"),
            P("tp", None),
            P(),
            P(("dp", "kv"), "tp", None),
            P(("dp", "kv"), "tp", None),
            P("tp", ("dp", "kv")),
            P(("dp", "kv"), None, "tp", None),
            P(("dp", "kv"), None, "tp", None),
            P(("dp", "kv"), "tp", None),
            P(("dp", "kv")),
        ),
        out_specs=(P(("dp", "kv"), None), P(("dp", "kv"), None, None)),
        check_vma=False,
    )
```

```python
import functools
import math

import jax
import jax.numpy as jnp
from jax import lax
from jax.experimental import pallas as pl
from jax.experimental.pallas import tpu as pltpu
from jax.sharding import PartitionSpec as P

EPS = 1e-06
MESH = pl.DeviceIdType.MESH
F32 = jnp.float32
BF16 = jnp.bfloat16


def dot(a, b):
    return lax.dot_general(a, b, (((1,), (0,)), ((), ())), preferred_element_type=F32)


def dot_t(a, b):
    return lax.dot_general(a, b, (((1,), (1,)), ((), ())), preferred_element_type=F32)


def rms_scale(source, gain):
    return source * lax.rsqrt(jnp.mean(source * source, axis=-1, keepdims=True) + EPS) * gain


def running_sum(rows, period):
    count, lanes = rows.shape
    place = lax.broadcasted_iota(jnp.int32, (count, lanes), 0)
    place = place & (period - 1) if period & (period - 1) == 0 else lax.rem(place, period)
    step = 1
    while step < period:
        shifted = jnp.concatenate([jnp.zeros((step, lanes), F32), rows[: count - step]], axis=0)
        rows = rows + jnp.where(place >= step, shifted, 0.0)
        step *= 2
    return rows


def kernel(
    kv_count,
    tp_count,
    piece_tokens,
    dec_tokens,
    norm_gain,
    query_weight,
    key_weight,
    value_weight,
    gate_weight,
    gate_bias,
    out_weight,
    out_gain,
    past_keys,
    past_values,
    past_gate,
    dec_keys,
    dec_values,
    dec_gate,
    dec_lengths,
    piece_out,
    dec_out,
    v_piece,
    v_dec,
    v_gain,
    v_wq,
    v_wk,
    v_wv,
    v_wg,
    v_bias,
    v_wo,
    v_ogain,
    v_pk,
    v_pv,
    v_pgate,
    v_dk,
    v_dv,
    v_dgate,
    v_len,
    rows_x,
    q_split,
    run_split,
    att_split,
    q_send,
    q_all,
    run_send,
    run_all,
    part_send,
    part_all,
    dec_part,
    dec_parts,
    piece_part,
    piece_parts,
    in_sem,
    dk_sem,
    dv_sem,
    q_ssem,
    q_rsem,
    run_ssem,
    run_rsem,
    part_ssem,
    part_rsem,
    tpd_ssem,
    tpd_rsem,
    tpp_ssem,
    tpp_rsem,
):
    R = v_piece.shape[0]
    S, T, D = v_dec.shape
    H = v_bias.shape[1]
    HD = v_pk.shape[1]
    PL = v_pk.shape[0]
    DP = v_dk.shape[1]
    N = S * T
    groups = dk_sem.shape[0]
    G = S // groups
    scale = HD ** (-0.5)
    me = lax.axis_index("kv")
    core = lax.axis_index("tp")

    loads = {}
    pairs = [
        (piece_tokens, v_piece),
        (dec_tokens, v_dec),
        (norm_gain, v_gain),
        (query_weight, v_wq),
        (gate_weight, v_wg),
        (gate_bias, v_bias),
        (key_weight, v_wk),
        (value_weight, v_wv),
        (dec_gate, v_dgate),
        (dec_lengths, v_len),
        (past_gate, v_pgate),
        (past_keys, v_pk),
        (past_values, v_pv),
    ]
    late = [(out_weight, v_wo), (out_gain, v_ogain)]
    count = 0

    def start_load(src, dst):
        nonlocal count
        loads[id(dst)] = pltpu.make_async_copy(src, dst, in_sem.at[count])
        loads[id(dst)].start()
        count += 1

    for src, dst in pairs:
        start_load(src, dst)
    dec_loads = []
    for g in range(groups):
        part = pl.ds(g * G, G)
        ck = pltpu.make_async_copy(dec_keys.at[part], v_dk.at[part], dk_sem.at[g])
        cv = pltpu.make_async_copy(dec_values.at[part], v_dv.at[part], dv_sem.at[g])
        ck.start()
        cv.start()
        dec_loads.append((ck, cv))
    for src, dst in late:
        start_load(src, dst)

    def ready(name, *refs):
        with jax.named_scope(name):
            for ref in refs:
                loads[id(ref)].wait()

    def arrive(name, copies):
        with jax.named_scope(name):
            for copy in copies:
                copy.wait_recv()

    barrier = pltpu.get_barrier_semaphore()
    for i in range(1, kv_count):
        pl.semaphore_signal(
            barrier, inc=1, device_id={"kv": lax.rem(me + i, kv_count)}, device_id_type=MESH
        )
    for i in range(1, tp_count):
        pl.semaphore_signal(
            barrier, inc=1, device_id={"tp": lax.rem(core + i, tp_count)}, device_id_type=MESH
        )

    ready("w_tok", v_piece, v_dec, v_gain)
    rows_x[:R, :] = v_piece[...].astype(F32)
    for s in range(S):
        rows_x[R + s * T : R + (s + 1) * T, :] = v_dec[s].astype(F32)
    normed = rms_scale(rows_x[...], v_gain[...]).astype(BF16)
    ready("w_gate", v_wg, v_bias)
    logits = dot_t(normed, v_wg[...]) + v_bias[...]
    log_gates = jnp.minimum(logits, 0.0) - jnp.log1p(jnp.exp(-jnp.abs(logits)))
    log_gates = jnp.concatenate([log_gates, jnp.zeros((R + N, HD - H), F32)], axis=1)
    local_run = running_sum(log_gates[:R], R)
    dec_run = running_sum(log_gates[R:], T)
    run_send[...] = split_terms(local_run, H).astype(BF16)
    ready("w_wq", v_wq)
    queries = dot(normed, v_wq[...])
    q_send[...] = queries[:R].astype(BF16)
    with jax.named_scope("barrier"):
        pl.semaphore_wait(barrier, kv_count - 1 + tp_count - 1)

    def send(src, dst, ssem, rsem, i, peer):
        copy = pltpu.make_async_remote_copy(
            src_ref=src,
            dst_ref=dst.at[me],
            send_sem=ssem.at[i - 1],
            recv_sem=rsem.at[i - 1],
            device_id={"kv": peer},
            device_id_type=MESH,
        )
        copy.start()
        return copy

    places = [partner(me, i, kv_count) for i in range(1, kv_count)]
    far_first = range(kv_count - 1, 0, -1)
    run_copies = [
        send(run_send, run_all, run_ssem, run_rsem, i, places[i - 1]) for i in far_first
    ]
    q_copies = [
        send(q_send, q_all, q_ssem, q_rsem, i, places[i - 1]) for i in far_first
    ]
    q_all[me] = queries[:R].astype(BF16)
    run_all[me] = split_terms(local_run, H).astype(BF16)

    for h in range(H):
        q_split[pl.ds(h, N, stride=H), :] = queries[R:, h * HD : (h + 1) * HD]
        run_split[pl.ds(h, N, stride=H), :] = jnp.broadcast_to(dec_run[:, h : h + 1], (N, HD))
    ready("w_wkv", v_wk, v_wv)
    key_rows = dot(normed, v_wk[...]).astype(BF16)
    value_rows = dot(normed, v_wv[...]).astype(BF16)
    pad = -(R + N) % 128
    runs_t = jnp.transpose(
        jnp.concatenate([local_run, dec_run, jnp.zeros((pad, HD), F32)], axis=0)
    )
    local_t = runs_t[:H, :R]
    dec_t = runs_t[:H, R : R + N]

    qd = q_split[...].astype(BF16)
    new_bias = jnp.concatenate([dec_t] * N, axis=0)
    new_scores = dot_t(qd, key_rows[R:]) * scale + run_split[:, :1] - new_bias
    row_at = lax.broadcasted_iota(jnp.int32, (N * H, N), 0)
    col_at = lax.broadcasted_iota(jnp.int32, (N * H, N), 1)
    col_in = col_at & (T - 1) if T & (T - 1) == 0 else lax.rem(col_at, T)
    keep = (row_at >= H * col_at) & (row_at < H * (col_at - col_in + T))
    new_scores = jnp.where(keep, new_scores, -jnp.inf)

    ready("w_dgate", v_dgate, v_len)
    slot = lax.broadcasted_iota(jnp.int32, (H, DP), 1)

    def decode_group(g):
        ck, cv = dec_loads[g]
        lo, hi = g * G * T * H, (g + 1) * G * T * H
        with jax.named_scope("w_dk"):
            ck.wait()
        biases, scores = [], []
        for s in range(g * G, (g + 1) * G):
            length = v_len[:, s : s + 1]
            gate = v_dgate[s]
            last = jnp.sum(jnp.where(slot == length - 1, gate, 0.0), axis=1, keepdims=True)
            bias = jnp.where(slot < length, last - gate, -jnp.inf)
            biases.append(jnp.concatenate([bias] * T, axis=0))
            scores.append(dot_t(qd[s * T * H : (s + 1) * T * H], v_dk[s]))
        old = jnp.concatenate(scores, axis=0) * scale + run_split[lo:hi, :1]
        old = old + jnp.concatenate(biases, axis=0)
        new = new_scores[lo:hi]
        top = jnp.maximum(
            jnp.max(old, axis=1, keepdims=True), jnp.max(new, axis=1, keepdims=True)
        )
        old = jnp.exp(old - top)
        new = jnp.exp(new - top)
        total = jnp.sum(old, axis=1, keepdims=True) + jnp.sum(new, axis=1, keepdims=True)
        old = old.astype(BF16)
        with jax.named_scope("w_dv"):
            cv.wait()
        summed = jnp.concatenate(
            [
                dot(old[i * T * H : (i + 1) * T * H], v_dv[g * G + i])
                for i in range(G)
            ],
            axis=0,
        )
        summed = summed + dot(new.astype(BF16), value_rows[R:])
        att_split[lo:hi, :] = summed / total

    for g in range(groups):
        decode_group(g)

    M = kv_count * R
    ready("w_past", v_pgate, v_pk, v_pv)
    past_bias = jnp.concatenate(
        [jnp.broadcast_to(v_pgate[h : h + 1, :], (M, PL)) for h in range(H)], axis=0
    )
    col_place = me * R + lax.broadcasted_iota(jnp.int32, (M, R), 1)
    row_place = lax.broadcasted_iota(jnp.int32, (M, R), 0)
    causal = jnp.where(col_place <= row_place, 0.0, -jnp.inf)
    lane = lax.broadcasted_iota(jnp.int32, (M, HD), 1)
    arrive("r_run", run_copies)
    before = jnp.zeros((1, HD), F32)
    own_before = jnp.zeros((1, HD), F32)
    run_rows = []
    for d in range(kv_count):
        shard = join_terms(run_all[d].astype(F32), H)
        own_before = jnp.where(me == d, before, own_before)
        run_rows.append(shard + before)
        before = before + shard[R - 1 : R]
    rows_run = jnp.concatenate(run_rows, axis=0)
    row_bias = jnp.concatenate([rows_run[:, h : h + 1] for h in range(H)], axis=0)
    own_bias = jnp.concatenate(
        [
            causal - (local_t[h : h + 1, :] + own_before[:, h : h + 1])
            for h in range(H)
        ],
        axis=0,
    )
    arrive("r_q", q_copies)
    qp = jnp.concatenate(
        [q_all[:, :, h * HD : (h + 1) * HD].reshape(M, HD) for h in range(H)], axis=0
    )
    old = dot_t(qp, v_pk[...]) * scale + past_bias + row_bias
    new = dot_t(qp, key_rows[:R]) * scale + row_bias + own_bias
    top = jnp.maximum(jnp.max(old, axis=1, keepdims=True), jnp.max(new, axis=1, keepdims=True))
    old = jnp.exp(old - top)
    new = jnp.exp(new - top)
    total = jnp.sum(old, axis=1, keepdims=True) + jnp.sum(new, axis=1, keepdims=True)
    summed = dot(old.astype(BF16), v_pv[...]) + dot(new.astype(BF16), value_rows[:R])
    stats = jnp.zeros((M, HD), F32)
    for h in range(H):
        part = slice(h * M, (h + 1) * M)
        part_send[:, :, h * HD : (h + 1) * HD] = summed[part].astype(BF16).reshape(kv_count, R, HD)
        stats = jnp.where(lane == h, top[part], stats)
        stats = jnp.where(lane == H + h, total[part], stats)
    part_send[:, :, H * HD :] = split_terms(stats, 2 * H).astype(BF16).reshape(kv_count, R, HD)
    part_copies = [
        send(part_send.at[places[i - 1]], part_all, part_ssem, part_rsem, i, places[i - 1])
        for i in far_first
    ]
    part_all[me] = part_send[me]

    def to_cores(src, dst, ssem, rsem):
        copies = []
        for i in range(1, tp_count):
            copy = pltpu.make_async_remote_copy(
                src_ref=src,
                dst_ref=dst.at[i - 1],
                send_sem=ssem.at[i - 1],
                recv_sem=rsem.at[i - 1],
                device_id={"tp": lax.rem(core + i, tp_count)},
                device_id_type=MESH,
            )
            copy.start()
            copies.append(copy)
        return copies

    def finish(name, part, parts, copies):
        mixed = part[...].astype(F32)
        arrive(name, copies)
        for i in range(tp_count - 1):
            mixed = mixed + parts[i].astype(F32)
        return rms_scale(mixed, v_ogain[...])

    ready("w_wo", v_wo, v_ogain)
    dec_att = jnp.concatenate(
        [att_split[pl.ds(h, N, stride=H), :].astype(BF16) for h in range(H)], axis=1
    )
    dec_part[...] = dot(dec_att, v_wo[...]).astype(BF16)
    tpd_copies = to_cores(dec_part, dec_parts, tpd_ssem, tpd_rsem)

    final = finish("r_tpd", dec_part, dec_parts, tpd_copies)
    for s in range(S):
        dec_out[s] = final[s * T : (s + 1) * T].astype(BF16)

    arrive("r_part", part_copies)
    stat = [join_terms(part_all[d, :, H * HD :].astype(F32), 2 * H) for d in range(kv_count)]
    best = functools.reduce(jnp.maximum, stat)
    pieces = []
    weights = [jnp.exp(x[:, :H] - best[:, :H]) for x in stat]
    whole = functools.reduce(jnp.add, [x[:, H : 2 * H] * w for x, w in zip(stat, weights)])
    for h in range(H):
        mixed = functools.reduce(
            jnp.add,
            [
                part_all[d, :, h * HD : (h + 1) * HD].astype(F32) * weights[d][:, h : h + 1]
                for d in range(kv_count)
            ],
        )
        pieces.append((mixed / whole[:, h : h + 1]).astype(BF16))
    piece_att = jnp.concatenate(pieces, axis=1)
    piece_part[...] = dot(piece_att, v_wo[...]).astype(BF16)
    tpp_copies = to_cores(piece_part, piece_parts, tpp_ssem, tpp_rsem)

    piece_out[...] = finish("r_tpp", piece_part, piece_parts, tpp_copies).astype(BF16)
    with jax.named_scope("sends"):
        for copy in q_copies + run_copies + part_copies + tpd_copies + tpp_copies:
            copy.wait_send()


def partner(me, i, count):
    if count & (count - 1):
        return (me + i) % count
    other, bit = 0, 1
    while bit < count:
        other = other + bit * ((me // bit + i // bit) % 2)
        bit *= 2
    return other


def split_terms(x, step):
    high = x.astype(BF16).astype(F32)
    middle = (x - high).astype(BF16).astype(F32)
    low = x - high - middle
    return high + pltpu.roll(middle, step, 1) + pltpu.roll(low, 2 * step, 1)


def join_terms(x, step):
    lanes = x.shape[1]
    return x + pltpu.roll(x, lanes - step, 1) + pltpu.roll(x, lanes - 2 * step, 1)


def write_out(piece, dec, piece_out, dec_out, sems):
    copies = [
        pltpu.make_async_copy(dec, dec_out, sems.at[0]),
        pltpu.make_async_copy(piece, piece_out, sems.at[1]),
    ]
    for copy in copies:
        copy.start()
    for copy in copies:
        copy.wait()


def body(kv_count, tp_count, *args):
    (
        piece_tokens,
        dec_tokens,
        norm_gain,
        query_weight,
        key_weight,
        value_weight,
        gate_weight,
        gate_bias,
        out_weight,
        out_gain,
        past_keys,
        past_values,
        past_gate,
        dec_keys,
        dec_values,
        dec_gate,
        dec_lengths,
    ) = args
    R, D = piece_tokens.shape
    S, T, _ = dec_tokens.shape
    PL, kv_local, HD = past_keys.shape
    DP = dec_keys.shape[1]
    H = gate_bias.shape[0]
    assert kv_local == 1
    N = S * T
    operands = (
        piece_tokens,
        dec_tokens,
        norm_gain.reshape(1, D),
        query_weight,
        key_weight,
        value_weight,
        gate_weight.T,
        gate_bias.reshape(1, H),
        out_weight,
        out_gain.reshape(1, D),
        past_keys.reshape(PL, HD),
        past_values.reshape(PL, HD),
        past_gate,
        dec_keys.reshape(S, DP, HD),
        dec_values.reshape(S, DP, HD),
        dec_gate,
        dec_lengths.reshape(1, S),
    )
    groups = math.gcd(S, 3)
    kv_peers = max(kv_count - 1, 1)
    tp_peers = max(tp_count - 1, 1)
    vmem = pltpu.VMEM
    dma = pltpu.SemaphoreType.DMA
    scratch = [vmem(x.shape, x.dtype) for x in operands] + [
        vmem((R + N, D), F32),
        vmem((N * H, HD), F32),
        vmem((N * H, HD), F32),
        vmem((N * H, HD), F32),
        vmem((R, H * HD), BF16),
        vmem((kv_count, R, H * HD), BF16),
        vmem((R, HD), BF16),
        vmem((kv_count, R, HD), BF16),
        vmem((kv_count, R, (H + 1) * HD), BF16),
        vmem((kv_count, R, (H + 1) * HD), BF16),
        vmem((N, D), BF16),
        vmem((tp_peers, N, D), BF16),
        vmem((R, D), BF16),
        vmem((tp_peers, R, D), BF16),
        dma((len(operands),)),
        dma((groups,)),
        dma((groups,)),
    ]
    scratch += [dma((kv_peers,))] * 6 + [dma((tp_peers,))] * 4
    results = pl.pallas_call(
        functools.partial(kernel, kv_count, tp_count),
        out_shape=(vmem((R, D), BF16), vmem((S, T, D), BF16)),
        in_specs=[pl.BlockSpec(memory_space=pltpu.HBM)] * len(operands),
        out_specs=(pl.BlockSpec(memory_space=pltpu.VMEM),) * 2,
        scratch_shapes=scratch,
        compiler_params=pltpu.CompilerParams(collective_id=0, has_side_effects=True),
        name="layer",
    )(*operands)
    return pl.pallas_call(
        write_out,
        out_shape=(
            jax.ShapeDtypeStruct((R, D), BF16),
            jax.ShapeDtypeStruct((S, T, D), BF16),
        ),
        in_specs=[pl.BlockSpec(memory_space=vmem)] * 2,
        out_specs=(pl.BlockSpec(memory_space=pltpu.HBM),) * 2,
        scratch_shapes=[dma((2,))],
        name="write_out",
    )(*[pltpu.with_memory_space_constraint(x, vmem) for x in results])


def solution(mesh):
    return jax.shard_map(
        functools.partial(body, mesh.shape["kv"], mesh.shape["tp"]),
        mesh=mesh,
        in_specs=(
            P(("dp", "kv"), None),
            P(("dp", "kv"), None, None),
            P(),
            P(None, "tp"),
            P(None, "tp"),
            P(None, "tp"),
            P(None, "tp"),
            P("tp"),
            P("tp", None),
            P(),
            P(("dp", "kv"), "tp", None),
            P(("dp", "kv"), "tp", None),
            P("tp", ("dp", "kv")),
            P(("dp", "kv"), None, "tp", None),
            P(("dp", "kv"), None, "tp", None),
            P(("dp", "kv"), "tp", None),
            P(("dp", "kv")),
        ),
        out_specs=(P(("dp", "kv"), None), P(("dp", "kv"), None, None)),
        check_vma=False,
    )
```
